512 devices in a mesh: fs: 64 (over z, y), tp: 8 (over x, core).
Axes of the slice: x: 4, y: 4, z: 16, core: 2. Of those that a mesh axis runs over, the one named last changes fastest.
Arguments:
- fwd_input: bfloat16 [8192, 2048], P('fs'), may hold values from -6 to 6
- saved_input: bfloat16 [8192, 2048], P('fs'), may hold values from -16 to 16
- out_cotangent: bfloat16 [8192, 2048], P('fs'), may hold values from -16 to 16
- up_weight: bfloat16 [2048, 4096], P('fs', 'tp'), may hold values from -0.125 to 0.125
- down_weight: bfloat16 [4096, 2048], P('tp', 'fs'), may hold values from -0.09375 to 0.09375
- up_grad_sum: float32 [2048, 4096], P('fs', 'tp'), may hold values from -6 to 6
Outputs:
- layer_out: bfloat16 [8192, 2048], P('fs')
- input_grad: bfloat16 [8192, 2048], P('fs')
- up_grad_out: float32 [2048, 4096], P('fs', 'tp')
The draws below stay inside these ranges and needn't reach their ends.
All inputs are finite; a program needn't handle non-finite values.
Results may differ from the reference program's by a relative error of at most 0.013.
Values may be sent and summed in bfloat16 or wider, within the bound.
No kernel may reach another device: no remote copies, remote signals or barrier semaphores. Data moves between devices by JAX's collectives and lax.ppermute only.
A program may use at most 64 MiB of HBM per device.

```python
import jax
import jax.numpy as jnp
from jax import lax

D = 2048
FF = 4096
TOKENS = 8192
N_TP = 8


def spiked(entries, key, source, target, parts, factor):
    owner, partner = [(jnp.arange(entries.shape[axis_at]) // (entries.shape[axis_at] // parts)).reshape([-1 if axis == axis_at else 1 for axis in range(entries.ndim)]) for axis_at in (source, target)]
    chosen = jax.random.permutation(key, parts)[partner]
    strong = (owner == chosen) | (owner == (partner + parts // 2) % parts)
    return jnp.where(strong, factor * entries, entries)


def level_of(own_key, dims, cuts, least, top_value):
    loudness, own = 1.0, jax.random.fold_in(own_key, 6)
    for position, shards_of in cuts:
        steps = jnp.exp(jax.random.uniform(jax.random.fold_in(own, position), (shards_of,), jnp.float32, least / len(cuts), top_value / len(cuts)))
        loudness = loudness * jnp.repeat(steps, dims[position] // shards_of).reshape([-1 if axis == position else 1 for axis in range(len(dims))])
    return loudness


def centred(stream_key, dims, spread, limit, cuts=(), held_as=jnp.bfloat16):
    loudness = level_of(stream_key, dims, cuts, -0.22, 0.18) if cuts else 1.0
    drawn = jax.random.normal(stream_key, dims, jnp.float32) * spread * loudness
    return jnp.minimum(jnp.maximum(drawn, -limit), limit).astype(held_as)


def bell_draw_with(key, shape, scale, most, pieces, heavy, dtype=jnp.bfloat16):
    values = scale * jax.random.normal(key, shape, jnp.float32)
    if pieces:
        values = values * level_of(key, shape, pieces, -0.22, 0.18)
    return jnp.clip(spiked(values, jax.random.fold_in(key, 3), *heavy), -most, most).astype(dtype)


def setup_inputs(seed: int = 0) -> dict:
    splits = jax.random.split(jax.random.key(seed), 7)
    fwd_input = centred(splits[0], (TOKENS, D), 1.0, 6.0, ((0, 64),))
    saved_input = bell_draw_with(splits[1], (TOKENS, D), 1.0, 16.0, ((0, 64),), (0, 1, 64, 4.0))
    out_cotangent = bell_draw_with(splits[2], (TOKENS, D), 1.0, 16.0, ((0, 64),), (0, 1, 64, 4.0))
    up_weight = centred(splits[3], (D, FF), D ** -0.5, 0.125, ((0, 64), (1, 8)))
    down_weight = centred(splits[4], (FF, D), FF ** -0.5, 0.09375, ((0, 8), (1, 64)))
    up_grad_sum = centred(splits[5], (D, FF), 1.0, 6.0, ((0, 64), (1, 8)), jnp.float32)
    return {"fwd_input": fwd_input, "saved_input": saved_input, "out_cotangent": out_cotangent, "up_weight": up_weight, "down_weight": down_weight, "up_grad_sum": up_grad_sum}


def split_sum(left, right):
    block = right.shape[0] // N_TP
    running = jnp.zeros((left.shape[0], right.shape[1]), jnp.float32)
    for index in range(N_TP):
        partial_out = jnp.dot(left[:, index * block:(index + 1) * block], right[index * block:(index + 1) * block], preferred_element_type=jnp.float32)
        rounded = lax.optimization_barrier(partial_out.astype(jnp.bfloat16))
        running = running + rounded.astype(jnp.float32)
    return running.astype(jnp.bfloat16)


def reference(fwd_input, saved_input, out_cotangent, up_weight, down_weight, up_grad_sum):
    pre_fwd = jnp.dot(fwd_input, up_weight, preferred_element_type=jnp.float32)
    positive = jnp.maximum(pre_fwd, 0.0)
    hidden = (positive * positive).astype(jnp.bfloat16)
    layer_out = split_sum(hidden, down_weight)
    pre_bwd = jnp.dot(saved_input, up_weight, preferred_element_type=jnp.float32)
    d_hidden = jnp.dot(out_cotangent, down_weight.T, preferred_element_type=jnp.float32)
    d_pre = (d_hidden * 2.0 * jnp.maximum(pre_bwd, 0.0)).astype(jnp.bfloat16)
    input_grad = split_sum(d_pre, up_weight.T)
    up_grad = jnp.dot(saved_input.T, d_pre, preferred_element_type=jnp.float32)
    up_grad_out = up_grad_sum + up_grad * (float(TOKENS) ** -0.5)
    return layer_out, input_grad, up_grad_out
```

```python
import jax
import jax.numpy as jnp
from jax import lax
from jax.sharding import PartitionSpec as P

NZ, NY = 16, 4
BOTH = ("fs", "tp")


def group_lists(n_tp):
    def device(z, y, t):
        return ((z % NZ) * NY + y % NY) * n_tp + t

    far = [
        [device(2 * i + a, 2 * j + b, t) for i in range(NZ // 2) for j in range(NY // 2)]
        for a in range(2)
        for b in range(2)
        for t in range(n_tp)
    ]
    near = []
    for t in range(n_tp):
        c = t % 2
        for r in range(NZ // 2):
            for q in range(NY // 2):
                members = [
                    (2 * r + c + dz, 2 * q + c + dy) for dz in range(2) for dy in range(2)
                ]
                members.sort(key=lambda m: (m[0] % 2, m[1] % 2))
                near.append([device(z, y, t) for z, y in members])
    return far, near


def exchange(array, groups):
    return lax.all_to_all(array, BOTH, 0, 0, axis_index_groups=groups, tiled=True)


def copies(array, n):
    return jnp.broadcast_to(array[None], (n, *array.shape))


def dot(a, b, dims):
    return lax.dot_general(a, b, (dims, ((), ())), preferred_element_type=jnp.float32)


def solution(mesh):
    n_tp = mesh.shape["tp"]
    n_fs = mesh.shape["fs"]
    far, near = group_lists(n_tp)
    n_far, n_near = len(far[0]), len(near[0])

    def per_device(fwd_input, saved_input, out_cotangent, up_weight, down_weight, up_grad_sum):
        rows, width = fwd_input.shape
        own, block = up_weight.shape
        bf16, f32 = jnp.bfloat16, jnp.float32
        w = jnp.concatenate([up_weight, down_weight.T], axis=0)
        w = exchange(copies(w, n_far), far)
        s = saved_input.reshape(rows, NZ // 2, 2, NY // 2, 2, own)
        s = s.transpose(2, 4, 0, 1, 3, 5).reshape(n_near, rows, n_far * own)
        w = w.reshape(n_far * 2 * own, block)
        packed = exchange(jnp.concatenate([copies(w, n_near), s], axis=1), near)
        w = packed[:, : n_far * 2 * own].reshape(2, 2, NZ // 2, NY // 2, 2, own, block)
        w = w.transpose(4, 2, 0, 3, 1, 5, 6).reshape(2, width, block)
        up, down_t = w[0], w[1]
        s = packed[:, n_far * 2 * own :].reshape(n_near * rows, n_far * own)

        pre_bwd = dot(saved_input, up, ((1,), (0,)))
        d_hidden = dot(out_cotangent, down_t, ((1,), (0,)))
        d_pre = (d_hidden * 2.0 * jnp.maximum(pre_bwd, 0.0)).astype(bf16)
        d_all = exchange(copies(d_pre, n_near), near).reshape(n_near * rows, block)

        pre_fwd = dot(fwd_input, up, ((1,), (0,)))
        positive = jnp.maximum(pre_fwd, 0.0)
        hidden = (positive * positive).astype(bf16)
        out_part = dot(hidden, down_t, ((1,), (1,))).astype(bf16)
        in_part = dot(d_pre, up, ((1,), (1,))).astype(bf16)

        grad = dot(s, d_all, ((0,), (0,))).astype(bf16).reshape(n_far, own, block)
        grad = exchange(grad, far).astype(f32).sum(axis=0)
        scale = float(rows * n_fs) ** (-0.5)
        up_grad_out = up_grad_sum + grad * scale

        piece = rows // n_tp
        parts = jnp.stack(
            [out_part.reshape(n_tp, piece, width), in_part.reshape(n_tp, piece, width)], axis=1
        )
        parts = lax.all_to_all(parts, "tp", 0, 0, tiled=True)
        sums = parts.astype(f32).sum(axis=0).astype(bf16)
        sums = lax.all_to_all(copies(sums, n_tp), "tp", 0, 0, tiled=True)
        layer_out = sums[:, 0].reshape(rows, width)
        input_grad = sums[:, 1].reshape(rows, width)
        return layer_out, input_grad, up_grad_out

    split = P("fs", None)
    in_specs = (split, split, split, P("fs", "tp"), P("tp", "fs"), P("fs", "tp"))
    return jax.shard_map(
        per_device,
        mesh=mesh,
        in_specs=in_specs,
        out_specs=(split, split, P("fs", "tp")),
        check_vma=False,
    )
```

```python
import jax
import jax.numpy as jnp
from jax import lax
from jax.experimental import pallas as pl
from jax.experimental.pallas import tpu as pltpu
from jax.sharding import PartitionSpec as P

NZ, NY = 16, 4
BOTH = ("fs", "tp")
BF16, F32 = jnp.bfloat16, jnp.float32


def group_lists(n_tp):
    def device(m, t):
        return ((m[0] % NZ) * NY + m[1] % NY) * n_tp + t

    def listed(members, key, t):
        return [device(m, t) for m in sorted(members, key=key)]

    def half_bits(m):
        return (m[0] % NZ) // 2 % 2, (m[1] % NY) // 2

    def low_bits(m):
        return m[0] % 2, m[1] % 2

    stride, middle, near, far = [], [], [], []
    for t in range(n_tp):
        c = t % 2
        for z in range(4):
            for y in range(NY):
                stride.append([device((4 * k + z, y), t) for k in range(NZ // 4)])
        for b in range(NZ // 4):
            for a in range(2):
                for q in range(2):
                    z = 4 * b + 2 * c + a
                    members = [(z + dz, q + dy) for dz in (0, 2) for dy in (0, 2)]
                    middle.append(listed(members, half_bits, t))
        for r in range(NZ // 2):
            for q in range(NY // 2):
                members = [(2 * r + c + dz, 2 * q + c + dy) for dz in (0, 1) for dy in (0, 1)]
                near.append(listed(members, low_bits, t))
        for a in range(2):
            for q in range(2):
                members = [(2 * i + a, 2 * j + q) for i in range(NZ // 2) for j in range(NY // 2)]
                far.append(listed(members, lambda m: (*half_bits(m), m[0] // 4), t))
    return stride, middle, near, far


def exchange(array, groups):
    return lax.all_to_all(array, BOTH, 0, 0, axis_index_groups=groups, tiled=True)


def copies(array, n):
    return jnp.broadcast_to(array[None], (n, *array.shape))


def to_classes(array, own):
    rows = array.shape[0]
    array = array.reshape(rows, NZ // 4, 2, 2, 2, 2, own)
    return array.transpose(0, 3, 5, 2, 4, 1, 6).reshape(rows, -1)


def from_classes(array, own):
    lead = array.shape[:-1]
    array = array.reshape(-1, 2, 2, 2, 2, NZ // 4, own)
    return array.transpose(0, 5, 3, 1, 4, 2, 6).reshape(*lead, -1)


def blocks_of(w_ref, b, which, n_far):
    both = w_ref[b, : 2 * n_far]
    both = both.reshape(n_far, 2, *both.shape[1:])[:, which]
    return both.reshape(-1, both.shape[-1])


def nn(a, b):
    return jnp.dot(a, b, preferred_element_type=F32)


def nt(a, b):
    return lax.dot_general(a, b, (((1,), (1,)), ((), ())), preferred_element_type=F32)


def d_pre_kernel(n_far, w_ref, saved_ref, cot_ref, out_ref):
    width = n_far * w_ref.shape[2]
    pre = d_hidden = 0.0
    for b in range(w_ref.shape[0]):
        cols = slice(b * width, (b + 1) * width)
        pre = pre + nn(saved_ref[:, cols], blocks_of(w_ref, b, 0, n_far))
        d_hidden = d_hidden + nn(cot_ref[:, cols], blocks_of(w_ref, b, 1, n_far))
    out_ref[...] = (d_hidden * 2.0 * jnp.maximum(pre, 0.0)).astype(BF16)


def parts_kernel(n_far, where_ref, w_ref, fwd_ref, d_pre_ref, mine_ref, other_ref, hid, dpr, left):
    width = n_far * w_ref.shape[2]
    pre = 0.0
    for b in range(w_ref.shape[0]):
        cols = slice(b * width, (b + 1) * width)
        pre = pre + nn(fwd_ref[:, cols], blocks_of(w_ref, b, 0, n_far))
    positive = jnp.maximum(pre, 0.0)
    hid[...] = (positive * positive).astype(BF16)
    dpr[...] = d_pre_ref[...]
    n_x, piece = mine_ref.shape[0], mine_ref.shape[2]
    for i, src in enumerate((hid, dpr)):
        for h in range(2):
            for k in range(n_x):
                core = lax.rem(where_ref[0] + h, 2)
                chip = lax.rem(where_ref[1] + k, n_x)
                row = pl.multiple_of((core * n_x + chip) * piece, piece)
                at = (h * n_x + k) * piece
                left[i, at : at + piece] = src[pl.ds(row, piece)]
    for i in range(2):
        a = left[i]
        for b in range(w_ref.shape[0]):
            cols = slice(b * width, (b + 1) * width)
            part = nt(a, blocks_of(w_ref, b, 1 - i, n_far)).astype(BF16)
            part = part.reshape(2, n_x, piece, width)
            mine_ref[:, i, :, cols] = part[0]
            other_ref[:, i, :, cols] = part[1]


def grad_kernel(n_far, w_ref, d_ref, out_ref):
    total = 0.0
    for b in range(w_ref.shape[0]):
        s = w_ref[b, 2 * n_far :]
        s = s.reshape(-1, s.shape[-1])
        total = total + lax.dot_general(
            s, d_ref[b], (((0,), (0,)), ((), ())), preferred_element_type=F32
        )
    out_ref[...] = total.astype(BF16).reshape(out_ref.shape)


def place_kernel(where_ref, own_ref, peer_ref, out_ref, in_ref):
    n_x, piece = own_ref.shape[0], own_ref.shape[2]
    for h, src in enumerate((own_ref, peer_ref)):
        for k in range(n_x):
            core = lax.rem(where_ref[0] + h, 2)
            chip = lax.rem(where_ref[1] + n_x - k, n_x)
            row = pl.multiple_of((core * n_x + chip) * piece, piece)
            out_ref[pl.ds(row, piece)] = src[k, 0]
            in_ref[pl.ds(row, piece)] = src[k, 1]


VMEM = pl.BlockSpec(memory_space=pltpu.VMEM)
SMEM = pl.BlockSpec(memory_space=pltpu.SMEM)


def call(kernel, outs, in_specs, args, flops, name, scratch=()):
    return pl.pallas_call(
        kernel,
        out_shape=outs,
        in_specs=in_specs,
        out_specs=jax.tree.map(lambda _: VMEM, outs),
        scratch_shapes=list(scratch),
        cost_estimate=pl.CostEstimate(flops=flops, bytes_accessed=1 << 22, transcendentals=0),
        name=name,
    )(*args)


def solution(mesh):
    n_tp = mesh.shape["tp"]
    n_fs = mesh.shape["fs"]
    n_x = n_tp // 2
    stride, middle, near, far = group_lists(n_tp)
    n_far, n_near = len(far[0]), len(near[0])
    swap = [(t, t ^ 1) for t in range(n_tp)]

    def to_right(k):
        return [(t, ((t // 2 + k) % n_x) * 2 + t % 2) for t in range(n_tp)]

    def per_device(fwd_input, saved_input, out_cotangent, up_weight, down_weight, up_grad_sum):
        rows, width = fwd_input.shape
        own, block = up_weight.shape
        piece = rows // n_tp
        shape = jax.ShapeDtypeStruct
        t = lax.axis_index("tp")
        where = jnp.stack([t % 2, t // 2]).astype(jnp.int32)

        w = jnp.concatenate([up_weight, down_weight.T], axis=0)
        w = exchange(copies(w, len(stride[0])), stride).reshape(-1, block)
        w = exchange(copies(w, len(middle[0])), middle).reshape(-1, block)
        fwd = to_classes(fwd_input, own)
        saved = to_classes(saved_input, own)
        cot = to_classes(out_cotangent, own)
        s = saved.reshape(rows, n_near, -1).transpose(1, 0, 2)
        w = exchange(jnp.concatenate([copies(w, n_near), s], axis=1), near)
        w = w.reshape(n_near, -1, own, block)

        one = 2 * rows * width * block
        d_pre = call(
            lambda *r: d_pre_kernel(n_far, *r), shape((rows, block), BF16), [VMEM] * 3,
            (w, saved, cot), 2 * one, "d_pre",
        )
        d_all = exchange(copies(d_pre, n_near), near)
        parts = shape((n_x, 2, piece, width), BF16)
        mine, other = call(
            lambda *r: parts_kernel(n_far, *r), (parts, parts), [SMEM, VMEM, VMEM, VMEM],
            (where, w, fwd, d_pre), 3 * one, "parts",
            [pltpu.VMEM((rows, block), BF16)] * 2 + [pltpu.VMEM((2, rows, block), BF16)],
        )
        other = lax.ppermute(other, "tp", swap)

        grad = call(
            lambda *r: grad_kernel(n_far, *r), shape((n_far, own, block), BF16), [VMEM] * 2,
            (w, d_all), one, "grad",
        )
        grad = exchange(grad, far)

        mine = (mine.astype(F32) + other.astype(F32)).astype(BF16)
        got = [mine[0]] + [lax.ppermute(mine[k], "tp", to_right(k)) for k in range(1, n_x)]
        total = sum(g.astype(F32) for g in got).astype(BF16)
        total = from_classes(total, own)
        got = [total] + [lax.ppermute(total, "tp", to_right(k)) for k in range(1, n_x)]
        got = jnp.stack(got)
        peer = lax.ppermute(got, "tp", swap)
        outs = shape((rows, width), BF16)
        layer_out, input_grad = call(
            place_kernel, (outs, outs), [SMEM, VMEM, VMEM], (where, got, peer), one // 8, "place"
        )

        scale = float(rows * n_fs) ** (-0.5)
        up_grad_out = up_grad_sum + grad.astype(F32).sum(axis=0) * scale
        return layer_out, input_grad, up_grad_out

    split = P("fs", None)
    return jax.shard_map(
        per_device,
        mesh=mesh,
        in_specs=(split, split, split, P("fs", "tp"), P("tp", "fs"), P("fs", "tp")),
        out_specs=(split, split, P("fs", "tp")),
        check_vma=False,
    )
```

```python
import jax
import jax.numpy as jnp
from jax import lax
from jax.experimental import pallas as pl
from jax.experimental.pallas import tpu as pltpu
from jax.sharding import PartitionSpec as P

NZ, NY = 16, 4
BOTH = ("fs", "tp")
BF16, F32 = jnp.bfloat16, jnp.float32


def group_lists(n_tp):
    def device(m, t):
        return ((m[0] % NZ) * NY + m[1] % NY) * n_tp + t

    def listed(members, key, t):
        return [device(m, t) for m in sorted(members, key=key)]

    def half_bits(m):
        return (m[0] % NZ) // 2 % 2, (m[1] % NY) // 2

    def low_bits(m):
        return m[0] % 2, m[1] % 2

    stride, middle, near, far = [], [], [], []
    for t in range(n_tp):
        c = t % 2
        for z in range(4):
            for y in range(NY):
                stride.append([device((4 * k + z, y), t) for k in range(NZ // 4)])
        for b in range(NZ // 4):
            for a in range(2):
                for q in range(2):
                    z = 4 * b + 2 * c + a
                    members = [(z + dz, q + dy) for dz in (0, 2) for dy in (0, 2)]
                    middle.append(listed(members, half_bits, t))
        for r in range(NZ // 2):
            for q in range(NY // 2):
                members = [(2 * r + c + dz, 2 * q + c + dy) for dz in (0, 1) for dy in (0, 1)]
                near.append(listed(members, low_bits, t))
        for a in range(2):
            for q in range(2):
                members = [(2 * i + a, 2 * j + q) for i in range(NZ // 2) for j in range(NY // 2)]
                far.append(listed(members, lambda m: (*half_bits(m), m[0] // 4), t))
    return stride, middle, near, far


def exchange(array, groups):
    return lax.all_to_all(array, BOTH, 0, 0, axis_index_groups=groups, tiled=True)


def copies(array, n):
    return jnp.broadcast_to(array[None], (n, *array.shape))


def to_classes(array, own):
    rows = array.shape[0]
    array = array.reshape(rows, NZ // 4, 2, 2, 2, 2, own)
    return array.transpose(0, 3, 5, 2, 4, 1, 6).reshape(rows, -1)


def from_classes(array, own):
    lead = array.shape[:-1]
    array = array.reshape(-1, 2, 2, 2, 2, NZ // 4, own)
    return array.transpose(0, 5, 3, 1, 4, 2, 6).reshape(*lead, -1)


def rows_of(w_ref, first, count, which):
    both = w_ref[2 * first : 2 * (first + count)]
    both = both.reshape(count, 2, *both.shape[1:])[:, which]
    return both.reshape(-1, both.shape[-1])


def nn(a, b):
    return jnp.dot(a, b, preferred_element_type=F32)


def nt(a, b):
    return lax.dot_general(a, b, (((1,), (1,)), ((), ())), preferred_element_type=F32)


def halves(half, own, *pairs):
    for h in range(2):
        yield 0, h, own, h * half
    for offset, pair in zip((1, 2, 3), pairs):
        for h in range(2):
            yield offset, h, pair[h], 0


def columns(where_ref, offset, h, width):
    start = (lax.bitwise_xor(where_ref[2], offset) * 2 + h) * width
    return pl.ds(pl.multiple_of(start, width), width)


def products(half, where_ref, held, xs_ref, cot_ref, pre, d_hidden):
    for offset, h, ref, first in held:
        cols = columns(where_ref, offset, h, half * ref.shape[1])
        pre = pre + nn(xs_ref[:, cols], rows_of(ref, first, half, 0))
        d_hidden = d_hidden + nn(cot_ref[:, cols], rows_of(ref, first, half, 1))
    return pre, d_hidden


def first_kernel(half, where_ref, xs_ref, cot_ref, own, y0, y1, z0, z1, pre_ref, d_hidden_ref):
    held = halves(half, own, (y0, y1), (z0, z1))
    pre_ref[...], d_hidden_ref[...] = products(half, where_ref, held, xs_ref, cot_ref, 0.0, 0.0)


def second_kernel(half, n_x, where_ref, xs_ref, cot_ref, v0, v1, pre_ref, d_hidden_ref, out_ref, left_ref, hid, dpr):
    held = ((3, h, v, 0) for h, v in enumerate((v0, v1)))
    pre, d_hidden = products(
        half, where_ref, held, xs_ref, cot_ref, pre_ref[...], d_hidden_ref[...]
    )
    rows = d_hidden.shape[0]
    positive = jnp.maximum(pre[:rows], 0.0)
    hid[...] = (positive * positive).astype(BF16)
    dpr[...] = (d_hidden * 2.0 * jnp.maximum(pre[rows:], 0.0)).astype(BF16)
    for k in range(out_ref.shape[0]):
        out_ref[k] = dpr[...]
    piece = rows // (2 * n_x)
    for i, src in enumerate((hid, dpr)):
        for h in range(2):
            for k in range(n_x):
                core = lax.rem(where_ref[0] + h, 2)
                chip = lax.rem(where_ref[1] + k, n_x)
                row = pl.multiple_of((core * n_x + chip) * piece, piece)
                at = (h * n_x + k) * piece
                left_ref[i, at : at + piece] = src[pl.ds(row, piece)]


def parts_kernel(half, where_ref, left_ref, own, y0, y1, z0, z1, v0, v1, mine_ref, other_ref):
    n_x, piece = mine_ref.shape[0], mine_ref.shape[2]
    for offset, h, ref, first in halves(half, own, (y0, y1), (z0, z1), (v0, v1)):
        width = half * ref.shape[1]
        cols = columns(where_ref, offset, h, width)
        for i in range(2):
            part = nt(left_ref[i], rows_of(ref, first, half, 1 - i)).astype(BF16)
            part = part.reshape(2, n_x, piece, width)
            mine_ref[:, i, :, cols] = part[0]
            other_ref[:, i, :, cols] = part[1]


def grad_kernel(where_ref, d_ref, *refs):
    *pieces, out_ref = refs
    total = 0.0
    for k, s_ref in enumerate(pieces):
        d = d_ref[lax.bitwise_xor(where_ref[2], k)]
        total = total + lax.dot_general(
            s_ref[...], d, (((0,), (0,)), ((), ())), preferred_element_type=F32
        )
    out_ref[...] = total.astype(BF16).reshape(out_ref.shape)


def place_kernel(where_ref, own_ref, peer_ref, out_ref, in_ref):
    n_x, piece = own_ref.shape[0], own_ref.shape[2]
    for h, src in enumerate((own_ref, peer_ref)):
        for k in range(n_x):
            core = lax.rem(where_ref[0] + h, 2)
            chip = lax.rem(where_ref[1] + n_x - k, n_x)
            row = pl.multiple_of((core * n_x + chip) * piece, piece)
            out_ref[pl.ds(row, piece)] = src[k, 0]
            in_ref[pl.ds(row, piece)] = src[k, 1]


VMEM = pl.BlockSpec(memory_space=pltpu.VMEM)
SMEM = pl.BlockSpec(memory_space=pltpu.SMEM)


def call(kernel, outs, args, flops, name, scratch=()):
    return pl.pallas_call(
        kernel,
        out_shape=outs,
        in_specs=[SMEM if a.dtype == jnp.int32 else VMEM for a in args],
        out_specs=jax.tree.map(lambda _: VMEM, outs),
        scratch_shapes=list(scratch),
        cost_estimate=pl.CostEstimate(flops=flops, bytes_accessed=1 << 22, transcendentals=0),
        name=name,
    )(*args)


def solution(mesh):
    n_tp = mesh.shape["tp"]
    n_fs = mesh.shape["fs"]
    n_x = n_tp // 2
    stride, middle, near, far = group_lists(n_tp)
    n_far, n_near = len(far[0]), len(near[0])
    swap = [(t, t ^ 1) for t in range(n_tp)]
    beside = [[(g[i], g[i ^ k]) for g in near for i in range(n_near)] for k in range(n_near)]

    def to_right(k):
        return [(t, ((t // 2 + k) % n_x) * 2 + t % 2) for t in range(n_tp)]

    def per_device(fwd_input, saved_input, out_cotangent, up_weight, down_weight, up_grad_sum):
        rows, width = fwd_input.shape
        own, block = up_weight.shape
        piece = rows // n_tp
        shape = jax.ShapeDtypeStruct
        t, f = lax.axis_index("tp"), lax.axis_index("fs")
        my_class = (f // NY % 2) * 2 + f % 2
        where = jnp.stack([t % 2, t // 2, my_class]).astype(jnp.int32)

        xs = jnp.concatenate([to_classes(fwd_input, own), to_classes(saved_input, own)], axis=0)
        cot = to_classes(out_cotangent, own)
        part = width // n_near
        pieces = []
        for k in range(n_near):
            s = lax.dynamic_slice(xs, (rows, (my_class ^ k) * part), (rows, part))
            pieces.append(s if k == 0 else lax.ppermute(s, BOTH, beside[k]))

        w = jnp.concatenate([up_weight, down_weight.T], axis=0)
        w = exchange(copies(w, len(stride[0])), stride).reshape(-1, block)
        w, pieces, xs, cot = lax.optimization_barrier((w, pieces, xs, cot))
        w = exchange(copies(w, len(middle[0])), middle).reshape(-1, own, block)

        def across(array, k):
            return lax.ppermute(array, BOTH, beside[k])

        half = n_far // 2
        w0, w1 = w[: 2 * half], w[2 * half :]
        y0, z1 = across(w0, 1), across(w1, 2)
        y1, z0 = across(w1, 1), across(w0, 2)
        v0, v1 = across(y0, 2), across(z1, 1)

        one = 2 * rows * width * block
        pre, d_hidden = call(
            lambda *r: first_kernel(half, *r),
            (shape((2 * rows, block), F32), shape((rows, block), F32)),
            (where, xs, cot, w, y0, y1, z0, z1), 2 * one, "first",
        )
        d_pre, left = call(
            lambda *r: second_kernel(half, n_x, *r),
            (shape((n_near, rows, block), BF16), shape((2, rows, block), BF16)),
            (where, xs, cot, v0, v1, pre, d_hidden), one, "second",
            [pltpu.VMEM((rows, block), BF16)] * 2,
        )
        d_all = exchange(d_pre, near)
        parts = shape((n_x, 2, piece, width), BF16)
        mine, other = call(
            lambda *r: parts_kernel(half, *r), (parts, parts),
            (where, left, w, y0, y1, z0, z1, v0, v1), 2 * one, "parts",
        )
        other = lax.ppermute(other, "tp", swap)

        grad = call(
            grad_kernel, shape((n_far, own, block), BF16),
            (where, d_all, *pieces), one, "grad",
        )
        grad = exchange(grad, far)

        mine = (mine.astype(F32) + other.astype(F32)).astype(BF16)
        got = [mine[0]] + [lax.ppermute(mine[k], "tp", to_right(k)) for k in range(1, n_x)]
        total = sum(g.astype(F32) for g in got).astype(BF16)
        total = from_classes(total, own)
        got = [total] + [lax.ppermute(total, "tp", to_right(k)) for k in range(1, n_x)]
        got = jnp.stack(got)
        peer = lax.ppermute(got, "tp", swap)
        outs = shape((rows, width), BF16)
        layer_out, input_grad = call(
            place_kernel, (outs, outs), (where, got, peer), one // 8, "place"
        )

        scale = float(rows * n_fs) ** (-0.5)
        up_grad_out = up_grad_sum + grad.astype(F32).sum(axis=0) * scale
        return layer_out, input_grad, up_grad_out

    split = P("fs", None)
    return jax.shard_map(
        per_device,
        mesh=mesh,
        in_specs=(split, split, split, P("fs", "tp"), P("tp", "fs"), P("fs", "tp")),
        out_specs=(split, split, P("fs", "tp")),
        check_vma=False,
    )
```
